32 devices in a mesh: fs: 8 (over z, x), tp: 4 (over y, core).
Axes of the slice: x: 2, y: 2, z: 4, core: 2. Of those that a mesh axis runs over, the one named last changes fastest.
Arguments:
- normed_input: bfloat16 [5120, 2048], P('fs'), may hold values from -448 to 448
- key_cotangent: bfloat16 [5120, 512], P('fs', 'tp'), may hold values from -0.078125 to 0.078125
- value_cotangent: bfloat16 [5120, 1024], P('fs', 'tp'), may hold values from -0.078125 to 0.078125
- key_factor: bfloat16 [512, 128], P('tp'), may hold values from -2.8 to 2.8
- value_factor: bfloat16 [1024, 128], P('tp'), may hold values from -2.8 to 2.8
- key_weight: float32 [2048, 512], P('fs', 'tp'), may hold values from -0.125 to 0.125
- value_weight: float32 [2048, 1024], P('fs', 'tp'), may hold values from -0.125 to 0.125
- first_moments: float32 [2, 2048, 128], P(None, 'fs', 'tp'), may hold values from -0.6 to 0.6
- second_moments: float32 [2, 2048, 128], P(None, 'fs', 'tp'), may hold values from 0.001 to 0.1
Outputs:
- first_new: float32 [2, 2048, 128], P(None, 'fs', 'tp')
- second_new: float32 [2, 2048, 128], P(None, 'fs', 'tp')
- new_key_weight: float32 [2048, 512], P('fs', 'tp')
- new_value_weight: float32 [2048, 1024], P('fs', 'tp')
- key_copy: bfloat16 [2048, 512], P(None, 'tp')
- value_copy: bfloat16 [2048, 1024], P(None, 'tp')
The draws below stay inside these ranges and needn't reach their ends.
All inputs are finite; a program needn't handle non-finite values.
Results may differ from the reference program's by a relative error of at most 0.005.
Values may be sent and summed in bfloat16 or wider, within the bound.
A program may use at most 64 MiB of HBM per device.

```python
import math
import jax
import jax.numpy as jnp
from jax import lax

D = 2048
RANK = 128
TOK_DEV = 640
TOKENS = 5120
NK = 512
NV = 1024
N_FS = 8


def factor_draw(base_key, rows_total, salt_value):
    key_list = jax.random.split(jax.random.fold_in(base_key, salt_value), 2)
    column = jnp.arange(RANK).astype(jnp.float32) / RANK
    rough_scale = jax.random.uniform(key_list[0], (RANK,), jnp.float32, 0.7, 1.4)
    base_draw = jnp.clip(jax.random.normal(key_list[1], (rows_total, RANK), jnp.float32), -5.0, 5.0)
    column_ramp = 10.0 ** column
    return (0.04 * base_draw * (column_ramp * rough_scale)[None, :]).astype(jnp.bfloat16)


def draw_key_factor(key, part):
    return factor_draw(key, NK, 21)


def draw_value_factor(key, part):
    return factor_draw(key, NV, 22)


def draw_normed_input(key, part):
    key_list = jax.random.split(jax.random.fold_in(key, 11), 4)
    blocks = TOKENS // TOK_DEV
    column = jnp.arange(D).astype(jnp.float32) / D
    rough_scale = jax.random.uniform(key_list[0], (D,), jnp.float32, 0.7, 1.4)
    noise_draw = jnp.clip(jax.random.normal(key_list[1], (TOKENS, D), jnp.float32), -5.0, 5.0)
    column_ramp = 10.0 ** column
    partner = jax.random.permutation(key_list[3], blocks)
    token_block = jnp.arange(TOKENS) // TOK_DEV
    column_block = jnp.arange(D) // (D // blocks)
    boost_mask = jnp.where(partner[token_block][:, None] == column_block[None, :], 4.0, 1.0)
    return (noise_draw * (column_ramp * rough_scale)[None, :] * boost_mask).astype(jnp.bfloat16)


def shard_levels(own_key, shape, cuts, low, largest):
    def one(dim, parts):
        heights = jax.random.uniform(jax.random.fold_in(jax.random.fold_in(own_key, 6), dim), (parts,), jnp.float32, low / len(cuts), largest / len(cuts))
        return jnp.repeat(jnp.exp(heights), shape[dim] // parts).reshape((-1,) + (1,) * (len(shape) - dim - 1))

    gain = one(*cuts[0])
    for cut in cuts[1:]:
        gain = gain * one(*cut)
    return gain


def centred(own_key, dims, deviation, reach, cuts=(), held_as=jnp.bfloat16):
    array = deviation * jax.random.normal(own_key, dims, jnp.float32)
    if cuts:
        array = array * shard_levels(own_key, dims, cuts, -0.22, 0.18)
    return jnp.clip(array, -reach, reach).astype(held_as)


def setup_inputs(seed: int = 0) -> dict:
    streams_of = jax.random.split(jax.random.key(seed), 10)
    normed_input = draw_normed_input(jax.random.fold_in(streams_of[9], 71), 0)
    key_cotangent = centred(streams_of[1], (TOKENS, NK), (TOK_DEV * N_FS) ** -0.5, 0.078125, ((0, 8), (1, 4)))
    value_cotangent = centred(streams_of[2], (TOKENS, NV), (TOK_DEV * N_FS) ** -0.5, 0.078125, ((0, 8), (1, 4)))
    key_factor = draw_key_factor(jax.random.fold_in(streams_of[9], 71), 0)
    value_factor = draw_value_factor(jax.random.fold_in(streams_of[9], 71), 0)
    key_weight = centred(streams_of[5], (D, NK), D ** -0.5, 0.125, ((0, 8), (1, 4)), jnp.float32)
    value_weight = centred(streams_of[6], (D, NV), D ** -0.5, 0.125, ((0, 8), (1, 4)), jnp.float32)
    first_moments = centred(streams_of[7], (2, D, RANK), 0.1, 0.6, ((1, 8), (2, 4)), jnp.float32)
    second_moments = jnp.clip(jnp.exp(math.log(0.1) - 4.6051702 * jax.random.uniform(streams_of[8], (2, D, RANK), jnp.float32) ** shard_levels(streams_of[8], (2, D, RANK), ((1, 8), (2, 4)), -0.2, 0.2)), 0.001, 0.1)
    return {"normed_input": normed_input, "key_cotangent": key_cotangent, "value_cotangent": value_cotangent, "key_factor": key_factor, "value_factor": value_factor, "key_weight": key_weight, "value_weight": value_weight, "first_moments": first_moments, "second_moments": second_moments}


step_rate = 0.05
clip_target = 0.1
beta_first = 0.8
beta_second = 0.95
small_eps = 1e-08
norm_eps = 1e-06

def reference(normed_input, key_cotangent, value_cotangent, key_factor, value_factor, key_weight, value_weight, first_moments, second_moments):
    contract = (((0,), (0,)), ((), ()))
    grad_key = lax.dot_general(normed_input, key_cotangent, contract, preferred_element_type=jnp.float32)
    grad_value = lax.dot_general(normed_input, value_cotangent, contract, preferred_element_type=jnp.float32)
    proj_key = jnp.dot(grad_key, key_factor.astype(jnp.float32), precision=lax.Precision.HIGHEST)
    proj_value = jnp.dot(grad_value, value_factor.astype(jnp.float32), precision=lax.Precision.HIGHEST)
    total_sq = jnp.sum(proj_key * proj_key) + jnp.sum(proj_value * proj_value)
    clip_limit = clip_target * jnp.sqrt(jnp.float32(2 * D * RANK))
    clip_factor = jnp.minimum(1.0, clip_limit / jnp.sqrt(total_sq + norm_eps))
    scaled = clip_factor * jnp.stack([proj_key, proj_value])
    first_new = beta_first * first_moments + (1.0 - beta_first) * scaled
    second_new = beta_second * second_moments + (1.0 - beta_second) * scaled * scaled
    direction = first_new / (jnp.sqrt(second_new) + small_eps)
    back = (((1,), (1,)), ((), ()))
    update_key = lax.dot_general(direction[0], key_factor.astype(jnp.float32), back, precision=lax.Precision.HIGHEST)
    update_value = lax.dot_general(direction[1], value_factor.astype(jnp.float32), back, precision=lax.Precision.HIGHEST)
    new_key = key_weight - step_rate * update_key
    new_value = value_weight - step_rate * update_value
    return (first_new, second_new, new_key, new_value, new_key.astype(jnp.bfloat16), new_value.astype(jnp.bfloat16))
```

```python
import functools

import jax
import jax.numpy as jnp
from jax import lax
from jax.experimental import pallas as pl
from jax.experimental.pallas import tpu as pltpu
from jax.sharding import PartitionSpec as P

step_rate = 0.05
clip_target = 0.1
beta_first = 0.8
beta_second = 0.95
small_eps = 1e-08
norm_eps = 1e-06

MESH = pl.DeviceIdType.MESH
BF16 = jnp.bfloat16
F32 = jnp.float32


def flip(a):
    return jnp.transpose(a.astype(F32))


def kernel(
    n_fs,
    n_tp,
    x_hbm,
    dk_ref,
    dv_ref,
    kf_ref,
    vf_ref,
    wk_ref,
    wv_ref,
    fm_ref,
    sm_ref,
    first_ref,
    second_ref,
    newk_ref,
    newv_ref,
    kcopy_ref,
    vcopy_ref,
    x_ref,
    part_ref,
    partin_ref,
    tok_ref,
    tokin_ref,
    sq_ref,
    sqin_ref,
    gat_ref,
    wall_ref,
    x_sem,
    part_ss,
    part_rs,
    tok_ss,
    tok_rs,
    sq_ss,
    sq_rs,
    gf_ss,
    gf_rs,
    gt_ss,
    gt_rs,
    w_ss,
    w_rs,
    wx_ss,
    wx_rs,
):
    fs = lax.axis_index("fs")
    tp = lax.axis_index("tp")
    n_dev = n_fs * n_tp
    lin = fs * n_tp + tp
    rank = kf_ref.shape[1]
    r = rank // n_tp
    rows = wk_ref.shape[0]
    nk = wk_ref.shape[1]
    nv = wv_ref.shape[1]
    model = x_ref.shape[1]
    pair = 2 if n_fs % 2 == 0 else 1
    n_far = n_fs // pair
    far = fs // pair
    near = fs % pair

    x_copy = pltpu.make_async_copy(x_hbm, x_ref, x_sem)
    x_copy.start()

    barrier = pltpu.get_barrier_semaphore()

    @pl.loop(1, n_dev)
    def _(k):
        other = lax.rem(lin + k, n_dev)
        pl.semaphore_signal(
            barrier,
            inc=1,
            device_id={"fs": other // n_tp, "tp": lax.rem(other, n_tp)},
            device_id_type=MESH,
        )

    kft = flip(kf_ref[...]).astype(BF16)
    vft = flip(vf_ref[...]).astype(BF16)
    last = (((1,), (1,)), ((), ()))
    red_k = lax.dot_general(kft, dk_ref[...], last, preferred_element_type=F32)
    red_v = lax.dot_general(vft, dv_ref[...], last, preferred_element_type=F32)
    for j in range(n_tp):
        part_ref[j, :r, :] = red_k[j * r : (j + 1) * r].astype(BF16)
        part_ref[j, r:, :] = red_v[j * r : (j + 1) * r].astype(BF16)
    wall_ref[fs, :, :nk] = wk_ref[...].astype(BF16)
    wall_ref[fs, :, nk:] = wv_ref[...].astype(BF16)

    pl.semaphore_wait(barrier, n_dev - 1)

    def part_copy(k):
        to = lax.rem(tp + k, n_tp)
        return pltpu.make_async_remote_copy(
            src_ref=part_ref.at[to],
            dst_ref=partin_ref.at[k - 1],
            send_sem=part_ss.at[k - 1],
            recv_sem=part_rs.at[k - 1],
            device_id={"tp": to},
            device_id_type=MESH,
        )

    parts = [part_copy(k) for k in range(1, n_tp)]
    for c in parts:
        c.start()

    def wall_copy(k):
        to = lax.rem(far + k, n_far) * pair + near
        return pltpu.make_async_remote_copy(
            src_ref=wall_ref.at[fs],
            dst_ref=wall_ref.at[fs],
            send_sem=w_ss.at[k - 1],
            recv_sem=w_rs.at[k - 1],
            device_id={"fs": to},
            device_id_type=MESH,
        )

    def wall_in(k):
        origin = lax.rem(far + n_far - k, n_far) * pair + near
        return pltpu.make_async_copy(
            wall_ref.at[origin], wall_ref.at[origin], w_rs.at[k - 1]
        )

    def wall_pair(k):
        block = lax.rem(far + n_far - k, n_far) * pair + near
        return pltpu.make_async_remote_copy(
            src_ref=wall_ref.at[block],
            dst_ref=wall_ref.at[block],
            send_sem=wx_ss.at[k],
            recv_sem=wx_rs.at[k],
            device_id={"fs": far * pair + 1 - near},
            device_id_type=MESH,
        )

    walls = [wall_copy(k) for k in range(1, n_far)]
    for c in walls:
        c.start()
    pairs = []
    if pair == 2:
        pairs.append(wall_pair(0))
        pairs[-1].start()

    fmt = jnp.concatenate([flip(fm_ref[0]), flip(fm_ref[1])], axis=0)
    smt = jnp.concatenate([flip(sm_ref[0]), flip(sm_ref[1])], axis=0)

    for c in parts:
        c.wait_recv()
    own = part_ref[tp].astype(F32)
    for k in range(1, n_tp):
        own = own + partin_ref[k - 1].astype(F32)
    own = own.astype(BF16)
    x_copy.wait()

    def tok_copy(c):
        return pltpu.make_async_remote_copy(
            src_ref=tok_ref.at[c],
            dst_ref=tokin_ref.at[fs],
            send_sem=tok_ss.at[c],
            recv_sem=tok_rs.at[fs],
            device_id={"fs": c},
            device_id_type=MESH,
        )

    width = max(rows, min(256, model))
    for base in range(0, model, width):
        prod = lax.dot_general(
            own,
            x_ref[:, base : base + width],
            (((1,), (0,)), ((), ())),
            preferred_element_type=F32,
        )
        for c in range(base // rows, (base + width) // rows):
            at = c * rows - base
            tok_ref[c] = prod[:, at : at + rows].astype(BF16)

            @pl.when(c != fs)
            def _():
                tok_copy(c).start()

    total = tok_ref[fs].astype(F32)
    for k in range(1, n_fs):
        origin = lax.rem(fs + k, n_fs)
        pltpu.make_async_copy(
            tokin_ref.at[origin], tokin_ref.at[origin], tok_rs.at[origin]
        ).wait()
        total = total + tokin_ref[origin].astype(F32)

    sq_ref[...] = jnp.full(sq_ref.shape, jnp.sum(total * total), F32)

    def sq_copy(k):
        other = lax.rem(lin + k, n_dev)
        return pltpu.make_async_remote_copy(
            src_ref=sq_ref,
            dst_ref=sqin_ref.at[k - 1],
            send_sem=sq_ss,
            recv_sem=sq_rs,
            device_id={"fs": other // n_tp, "tp": lax.rem(other, n_tp)},
            device_id_type=MESH,
        )

    @pl.loop(1, n_dev)
    def _(k):
        sq_copy(k).start()

    pltpu.make_async_copy(sqin_ref, sqin_ref, sq_rs).wait()
    total_sq = jnp.max(jnp.sum(sqin_ref[...], axis=0) + sq_ref[...])
    limit = clip_target * (2.0 * model * rank) ** 0.5
    clip_factor = jnp.minimum(
        1.0, limit / jnp.sqrt(jnp.full((1, 1), total_sq + norm_eps, F32))
    )
    scaled = clip_factor * total
    first_new = beta_first * fmt + (1.0 - beta_first) * scaled
    second_new = beta_second * smt + (1.0 - beta_second) * scaled * scaled
    direction = first_new / (jnp.sqrt(second_new) + small_eps)

    mine = pl.ds(pl.multiple_of(tp * r, r), r)
    gat_ref[fs, 0, mine, :] = direction[:r].astype(BF16)
    gat_ref[fs, 1, mine, :] = direction[r:].astype(BF16)

    def gat_copy(k):
        block = gat_ref.at[fs, :, mine, :]
        return pltpu.make_async_remote_copy(
            src_ref=block,
            dst_ref=block,
            send_sem=gf_ss.at[k - 1],
            recv_sem=gf_rs.at[k - 1],
            device_id={"fs": lax.rem(fs + k, n_fs)},
            device_id_type=MESH,
        )

    def gat_in(k):
        origin = lax.rem(fs + n_fs - k, n_fs)
        block = gat_ref.at[origin, :, mine, :]
        return pltpu.make_async_copy(block, block, gf_rs.at[k - 1])

    bits = []
    b = n_tp // 2
    while b:
        bits.append(b)
        b //= 2

    def flipped(v, bit):
        return v + bit - 2 * bit * (v // bit % 2)

    held = [[]]
    for bit in bits:
        held.append(held[-1] + [bit])

    def sources(step):
        out = [0]
        for bit in bits[:step]:
            out = out + [o + bit for o in out]
        return out

    def tp_of(mask):
        v = tp
        for bit in bits:
            if mask & bit:
                v = flipped(v, bit)
        return v

    def share_copy(k, step, mask):
        origin = lax.rem(fs + n_fs - k, n_fs)
        at = pl.ds(pl.multiple_of(tp_of(mask) * r, r), r)
        block = gat_ref.at[origin, :, at, :]
        slot = mask | bits[step]
        return pltpu.make_async_remote_copy(
            src_ref=block,
            dst_ref=block,
            send_sem=gt_ss.at[k, slot - 1],
            recv_sem=gt_rs.at[k, slot - 1],
            device_id={"tp": flipped(tp, bits[step])},
            device_id_type=MESH,
        )

    def share_in(k, slot):
        origin = lax.rem(fs + n_fs - k, n_fs)
        at = pl.ds(pl.multiple_of(tp_of(slot) * r, r), r)
        block = gat_ref.at[origin, :, at, :]
        return pltpu.make_async_copy(block, block, gt_rs.at[k, slot - 1])

    shares = []

    def share(k, step):
        for mask in sources(step):
            c = share_copy(k, step, mask)
            c.start()
            shares.append(c)

    gats = [gat_copy(k) for k in range(1, n_fs)]
    if bits:
        share(0, 0)
    for c in gats:
        c.start()

    for i in range(2):
        first_ref[i] = jnp.transpose(first_new[i * r : (i + 1) * r])
        second_ref[i] = jnp.transpose(second_new[i * r : (i + 1) * r])

    for k in range(1, n_far):
        wall_in(k).wait()
        if pair == 2:
            pairs.append(wall_pair(k))
            pairs[-1].start()

    order = list(range(n_fs))
    for k in order:
        if k:
            gat_in(k).wait()
            if bits:
                share(k, 0)
    for step in range(1, len(bits)):
        for k in order:
            for mask in sources(step - 1):
                share_in(k, mask | bits[step - 1]).wait()
            share(k, step)

    back = (((0,), (0,)), ((), ()))

    def update(block):
        up_k = lax.dot_general(gat_ref[block, 0], kft, back, preferred_element_type=F32)
        up_v = lax.dot_general(gat_ref[block, 1], vft, back, preferred_element_type=F32)
        return step_rate * up_k, step_rate * up_v

    for k in range(n_fs):
        origin = lax.rem(fs + n_fs - k, n_fs)
        if bits:
            for mask in sources(len(bits) - 1):
                share_in(k, mask | bits[-1]).wait()
        up_k, up_v = update(origin)
        at = pl.ds(pl.multiple_of(origin * rows, rows), rows)
        if k == 0:
            new_k = wk_ref[...] - up_k
            new_v = wv_ref[...] - up_v
            newk_ref[...] = new_k
            newv_ref[...] = new_v
            kcopy_ref[at, :] = new_k.astype(BF16)
            vcopy_ref[at, :] = new_v.astype(BF16)
        else:
            if k == 1:
                for m in range(n_far if pair == 2 else 0):
                    block = lax.rem(far + n_far - m, n_far) * pair + 1 - near
                    pltpu.make_async_copy(
                        wall_ref.at[block], wall_ref.at[block], wx_rs.at[m]
                    ).wait()
            kcopy_ref[at, :] = (wall_ref[origin, :, :nk].astype(F32) - up_k).astype(BF16)
            vcopy_ref[at, :] = (wall_ref[origin, :, nk:].astype(F32) - up_v).astype(BF16)

    for c in parts + walls + pairs + gats + shares:
        c.wait_send()
    for c in range(n_fs):

        @pl.when(c != fs)
        def _():
            tok_copy(c).wait_send()

    pltpu.make_async_copy(sqin_ref, sqin_ref, sq_ss).wait()


def local(n_fs, n_tp, *args):
    x, dk, dv, kf, vf, wk, wv, fm, sm = args
    tokens, model = x.shape
    rows, nk = wk.shape
    nv = wv.shape[1]
    rank = kf.shape[1]
    r = rank // n_tp
    n_dev = n_fs * n_tp
    dma = pltpu.SemaphoreType.DMA
    vmem = pl.BlockSpec(memory_space=pltpu.VMEM)
    pair = 2 if n_fs % 2 == 0 else 1
    n_far = n_fs // pair
    return pl.pallas_call(
        functools.partial(kernel, n_fs, n_tp),
        out_shape=(
            jax.ShapeDtypeStruct(fm.shape, F32),
            jax.ShapeDtypeStruct(sm.shape, F32),
            jax.ShapeDtypeStruct(wk.shape, F32),
            jax.ShapeDtypeStruct(wv.shape, F32),
            jax.ShapeDtypeStruct((model, nk), BF16),
            jax.ShapeDtypeStruct((model, nv), BF16),
        ),
        in_specs=[pl.BlockSpec(memory_space=pl.ANY)] + [vmem] * 8,
        out_specs=(vmem,) * 6,
        scratch_shapes=[
            pltpu.VMEM((tokens, model), BF16),
            pltpu.VMEM((n_tp, 2 * r, tokens), BF16),
            pltpu.VMEM((max(n_tp - 1, 1), 2 * r, tokens), BF16),
            pltpu.VMEM((n_fs, 2 * r, rows), BF16),
            pltpu.VMEM((n_fs, 2 * r, rows), BF16),
            pltpu.VMEM((8, 128), F32),
            pltpu.VMEM((n_dev - 1, 8, 128), F32),
            pltpu.VMEM((n_fs, 2, rank, rows), BF16),
            pltpu.VMEM((n_fs, rows, nk + nv), BF16),
            dma,
            dma((max(n_tp - 1, 1),)),
            dma((max(n_tp - 1, 1),)),
            dma((n_fs,)),
            dma((n_fs,)),
            dma,
            dma,
            dma((n_fs,)),
            dma((n_fs,)),
            dma((n_fs, n_tp)),
            dma((n_fs, n_tp)),
            dma((n_far,)),
            dma((n_far,)),
            dma((n_far,)),
            dma((n_far,)),
        ],
        compiler_params=pltpu.CompilerParams(
            collective_id=0, has_side_effects=True, vmem_limit_bytes=60 * 1024 * 1024
        ),
    )(*args)


def solution(mesh):
    placed = (
        P("fs", None),
        P("fs", "tp"),
        P("fs", "tp"),
        P("tp", None),
        P("tp", None),
        P("fs", "tp"),
        P("fs", "tp"),
        P(None, "fs", "tp"),
        P(None, "fs", "tp"),
    )
    return jax.shard_map(
        functools.partial(local, mesh.shape["fs"], mesh.shape["tp"]),
        mesh=mesh,
        in_specs=placed,
        out_specs=(
            P(None, "fs", "tp"),
            P(None, "fs", "tp"),
            P("fs", "tp"),
            P("fs", "tp"),
            P(None, "tp"),
            P(None, "tp"),
        ),
        check_vma=False,
    )
```

```python
import functools

import jax
import jax.numpy as jnp
from jax import lax
from jax.experimental import pallas as pl
from jax.experimental.pallas import tpu as pltpu
from jax.sharding import PartitionSpec as P

step_rate = 0.05
clip_target = 0.1
beta_first = 0.8
beta_second = 0.95
small_eps = 1e-08
norm_eps = 1e-06

MESH = pl.DeviceIdType.MESH
BF16 = jnp.bfloat16
F32 = jnp.float32


def flip(a):
    return jnp.transpose(a.astype(F32))


def start(c):
    c.start()


def finish(c):
    c.wait_send()


def kernel(n_fs, n_tp, *refs):
    hbm = refs[:9]
    gat_ref, wall_ref, first_ref, second_ref = refs[9:13]
    held_in = refs[13:22]
    x_ref, dk_ref, dv_ref, kf_ref, vf_ref, wk_ref, wv_ref, fm_ref, sm_ref = held_in
    part_ref, partin_ref, tok_ref, tokin_ref, sq_ref, sqin_ref = refs[22:28]
    in_sem, part_ss, part_rs, tok_ss, tok_rs, sq_ss, sq_rs = refs[28:35]
    gf_ss, gf_rs, gt_ss, gt_rs, w_ss, w_rs, wx_ss, wx_rs = refs[35:]
    fs = lax.axis_index("fs")
    tp = lax.axis_index("tp")
    n_dev = n_fs * n_tp
    lin = fs * n_tp + tp
    rank = kf_ref.shape[1]
    r = rank // n_tp
    rows = wk_ref.shape[0]
    nk = wk_ref.shape[1]
    nv = wv_ref.shape[1]
    model = x_ref.shape[1]
    pair = 2 if n_fs % 2 == 0 else 1
    n_far = n_fs // pair
    far = fs // pair
    near = fs % pair

    loads = [
        pltpu.make_async_copy(hbm[i], held_in[i], in_sem.at[i]) for i in range(9)
    ]
    for i in (3, 4, 1, 2, 5, 6, 0, 7, 8):
        loads[i].start()

    barrier = pltpu.get_barrier_semaphore()

    @pl.loop(1, n_dev)
    def _(k):
        other = lax.rem(lin + k, n_dev)
        pl.semaphore_signal(
            barrier,
            inc=1,
            device_id={"fs": other // n_tp, "tp": lax.rem(other, n_tp)},
            device_id_type=MESH,
        )

    for i in (3, 4, 1, 2):
        loads[i].wait()
    kft = flip(kf_ref[...]).astype(BF16)
    vft = flip(vf_ref[...]).astype(BF16)
    last = (((1,), (1,)), ((), ()))
    red_k = lax.dot_general(kft, dk_ref[...], last, preferred_element_type=F32)
    red_v = lax.dot_general(vft, dv_ref[...], last, preferred_element_type=F32)
    for j in range(n_tp):
        part_ref[j, :r, :] = red_k[j * r : (j + 1) * r].astype(BF16)
        part_ref[j, r:, :] = red_v[j * r : (j + 1) * r].astype(BF16)
    for i in (5, 6):
        loads[i].wait()
    wall_ref[fs, :, :nk] = wk_ref[...].astype(BF16)
    wall_ref[fs, :, nk:] = wv_ref[...].astype(BF16)

    pl.semaphore_wait(barrier, n_dev - 1)

    def part_copy(k):
        to = lax.rem(tp + k, n_tp)
        return pltpu.make_async_remote_copy(
            src_ref=part_ref.at[to],
            dst_ref=partin_ref.at[k - 1],
            send_sem=part_ss.at[k - 1],
            recv_sem=part_rs.at[k - 1],
            device_id={"tp": to},
            device_id_type=MESH,
        )

    parts = [part_copy(k) for k in range(1, n_tp)]
    for c in parts:
        c.start()

    def wall_hop(block_far, way):
        block = wall_ref.at[block_far * pair + near]
        return pltpu.make_async_remote_copy(
            src_ref=block,
            dst_ref=block,
            send_sem=w_ss.at[(way + 1) // 2, block_far],
            recv_sem=w_rs.at[block_far],
            device_id={"fs": (far + way) * pair + near},
            device_id_type=MESH,
        )

    def wall_pair(block_far):
        block = wall_ref.at[block_far * pair + near]
        return pltpu.make_async_remote_copy(
            src_ref=block,
            dst_ref=block,
            send_sem=wx_ss.at[block_far],
            recv_sem=wx_rs.at[block_far],
            device_id={"fs": far * pair + 1 - near},
            device_id_type=MESH,
        )

    def wall_step(d, act):
        for way in (1, -1):
            block_far = far - d * way
            here = (block_far >= 0) & (block_far < n_far)
            more = here & (far + way >= 0) & (far + way < n_far)
            if d == 0:
                if pair == 2 and way == 1:
                    act(wall_pair(far))
            else:

                @pl.when(here)
                def _():
                    block = wall_ref.at[block_far * pair + near]
                    if act is start:
                        pltpu.make_async_copy(block, block, w_rs.at[block_far]).wait()

            @pl.when(more)
            def _():
                act(wall_hop(block_far, way))

            if d and pair == 2:

                @pl.when(here)
                def _():
                    act(wall_pair(block_far))

    wall_step(0, start)

    for c in parts:
        c.wait_recv()
    own = part_ref[tp].astype(F32)
    for k in range(1, n_tp):
        own = own + partin_ref[k - 1].astype(F32)
    own = own.astype(BF16)
    loads[0].wait()

    def tok_copy(c):
        return pltpu.make_async_remote_copy(
            src_ref=tok_ref.at[c],
            dst_ref=tokin_ref.at[fs],
            send_sem=tok_ss.at[c],
            recv_sem=tok_rs.at[fs],
            device_id={"fs": c},
            device_id_type=MESH,
        )

    width = max(rows, min(256, model))
    for base in range(0, model, width):
        prod = lax.dot_general(
            own,
            x_ref[:, base : base + width],
            (((1,), (0,)), ((), ())),
            preferred_element_type=F32,
        )
        for c in range(base // rows, (base + width) // rows):
            at = c * rows - base
            tok_ref[c] = prod[:, at : at + rows].astype(BF16)

            @pl.when(c != fs)
            def _():
                tok_copy(c).start()

    if n_far > 1:
        wall_step(1, start)
    for i in (7, 8):
        loads[i].wait()
    fmt = fm_ref[...].reshape(2 * r, rows)
    smt = sm_ref[...].reshape(2 * r, rows)

    total = tok_ref[fs].astype(F32)
    for k in range(1, n_fs):
        origin = lax.rem(fs + k, n_fs)
        pltpu.make_async_copy(
            tokin_ref.at[origin], tokin_ref.at[origin], tok_rs.at[origin]
        ).wait()
        total = total + tokin_ref[origin].astype(F32)

    sq_ref[...] = jnp.full(sq_ref.shape, jnp.sum(total * total), F32)

    def sq_copy(k):
        other = lax.rem(lin + k, n_dev)
        return pltpu.make_async_remote_copy(
            src_ref=sq_ref,
            dst_ref=sqin_ref.at[k - 1],
            send_sem=sq_ss,
            recv_sem=sq_rs,
            device_id={"fs": other // n_tp, "tp": lax.rem(other, n_tp)},
            device_id_type=MESH,
        )

    @pl.loop(1, n_dev)
    def _(k):
        sq_copy(k).start()

    if n_far > 2:
        wall_step(2, start)
    pltpu.make_async_copy(sqin_ref, sqin_ref, sq_rs).wait()
    total_sq = jnp.max(jnp.sum(sqin_ref[...], axis=0) + sq_ref[...])
    limit = clip_target * (2.0 * model * rank) ** 0.5
    clip_factor = jnp.minimum(
        1.0, limit / jnp.sqrt(jnp.full((1, 1), total_sq + norm_eps, F32))
    )
    scaled = clip_factor * total
    first_new = beta_first * fmt + (1.0 - beta_first) * scaled
    second_new = beta_second * smt + (1.0 - beta_second) * scaled * scaled
    direction = first_new / (jnp.sqrt(second_new) + small_eps)

    mine = pl.ds(pl.multiple_of(tp * r, r), r)
    gat_ref[fs, 0, mine, :] = direction[:r].astype(BF16)
    gat_ref[fs, 1, mine, :] = direction[r:].astype(BF16)

    def gat_copy(k):
        block = gat_ref.at[fs, :, mine, :]
        return pltpu.make_async_remote_copy(
            src_ref=block,
            dst_ref=block,
            send_sem=gf_ss.at[k - 1],
            recv_sem=gf_rs.at[k - 1],
            device_id={"fs": lax.rem(fs + k, n_fs)},
            device_id_type=MESH,
        )

    def gat_in(k):
        origin = lax.rem(fs + n_fs - k, n_fs)
        block = gat_ref.at[origin, :, mine, :]
        return pltpu.make_async_copy(block, block, gf_rs.at[k - 1])

    bits = []
    b = n_tp // 2
    while b:
        bits.append(b)
        b //= 2

    def flipped(v, bit):
        return v + bit - 2 * bit * (v // bit % 2)

    held = [[]]
    for bit in bits:
        held.append(held[-1] + [bit])

    def sources(step):
        out = [0]
        for bit in bits[:step]:
            out = out + [o + bit for o in out]
        return out

    def tp_of(mask):
        v = tp
        for bit in bits:
            if mask & bit:
                v = flipped(v, bit)
        return v

    def share_copy(k, step, mask):
        origin = lax.rem(fs + n_fs - k, n_fs)
        at = pl.ds(pl.multiple_of(tp_of(mask) * r, r), r)
        block = gat_ref.at[origin, :, at, :]
        slot = mask | bits[step]
        return pltpu.make_async_remote_copy(
            src_ref=block,
            dst_ref=block,
            send_sem=gt_ss.at[k, slot - 1],
            recv_sem=gt_rs.at[k, slot - 1],
            device_id={"tp": flipped(tp, bits[step])},
            device_id_type=MESH,
        )

    def share_in(k, slot):
        origin = lax.rem(fs + n_fs - k, n_fs)
        at = pl.ds(pl.multiple_of(tp_of(slot) * r, r), r)
        block = gat_ref.at[origin, :, at, :]
        return pltpu.make_async_copy(block, block, gt_rs.at[k, slot - 1])

    shares = []

    def share(k, step):
        for mask in sources(step):
            c = share_copy(k, step, mask)
            c.start()
            shares.append(c)

    gats = [gat_copy(k) for k in range(1, n_fs)]
    if bits:
        share(0, 0)
    for c in gats:
        c.start()

    first_ref[...] = first_new.reshape(2, r, rows)
    second_ref[...] = second_new.reshape(2, r, rows)

    for d in range(3, n_far):
        wall_step(d, start)

    order = list(range(n_fs))
    for k in order:
        if k:
            gat_in(k).wait()
            if bits:
                share(k, 0)
    for step in range(1, len(bits)):
        for k in order:
            for mask in sources(step - 1):
                share_in(k, mask | bits[step - 1]).wait()
            share(k, step)

    for k in order:
        if bits:
            for mask in sources(len(bits) - 1):
                share_in(k, mask | bits[-1]).wait()
    if pair == 2:
        for m in range(n_far):
            block = wall_ref.at[m * pair + 1 - near]
            pltpu.make_async_copy(block, block, wx_rs.at[m]).wait()

    for c in parts + gats + shares:
        c.wait_send()
    for d in range(n_far):
        wall_step(d, finish)
    for c in range(n_fs):

        @pl.when(c != fs)
        def _():
            tok_copy(c).wait_send()

    pltpu.make_async_copy(sqin_ref, sqin_ref, sq_ss).wait()


def results(
    n_fs,
    gat_ref,
    wall_ref,
    first_in,
    second_in,
    kf_ref,
    vf_ref,
    wk_ref,
    wv_ref,
    first_ref,
    second_ref,
    newk_ref,
    newv_ref,
    kout_ref,
    vout_ref,
    kcopy_ref,
    vcopy_ref,
    k_sem,
    v_sem,
):
    fs = lax.axis_index("fs")
    rows, nk = wk_ref.shape
    back = (((0,), (0,)), ((), ()))
    kft = flip(kf_ref[...]).astype(BF16)
    vft = flip(vf_ref[...]).astype(BF16)
    first_ref[...] = first_in[...]
    second_ref[...] = second_in[...]

    def update(block):
        up_k = lax.dot_general(gat_ref[block, 0], kft, back, preferred_element_type=F32)
        up_v = lax.dot_general(gat_ref[block, 1], vft, back, preferred_element_type=F32)
        return step_rate * up_k, step_rate * up_v

    outs = []
    for k in range(n_fs):
        origin = lax.rem(fs + k, n_fs)
        up_k, up_v = update(origin)
        at = pl.ds(pl.multiple_of(origin * rows, rows), rows)
        if k == 0:
            new_k = wk_ref[...] - up_k
            new_v = wv_ref[...] - up_v
            newk_ref[...] = new_k
            newv_ref[...] = new_v
        else:
            new_k = wall_ref[origin, :, :nk].astype(F32) - up_k
            new_v = wall_ref[origin, :, nk:].astype(F32) - up_v
        kcopy_ref[k] = new_k.astype(BF16)
        vcopy_ref[k] = new_v.astype(BF16)
        for c in (
            pltpu.make_async_copy(kcopy_ref.at[k], kout_ref.at[at, :], k_sem.at[k]),
            pltpu.make_async_copy(vcopy_ref.at[k], vout_ref.at[at, :], v_sem.at[k]),
        ):
            c.start()
            outs.append(c)
    for c in outs:
        c.wait()


def local(n_fs, n_tp, x, dk, dv, kf, vf, wk, wv, fm, sm):
    tokens, model = x.shape
    rows, nk = wk.shape
    nv = wv.shape[1]
    rank = kf.shape[1]
    r = rank // n_tp
    n_dev = n_fs * n_tp
    dma = pltpu.SemaphoreType.DMA
    vmem = pl.BlockSpec(memory_space=pltpu.VMEM)
    anywhere = pl.BlockSpec(memory_space=pl.ANY)
    pair = 2 if n_fs % 2 == 0 else 1
    n_far = n_fs // pair
    peers = max(n_tp - 1, 1)
    args = (x, dk, dv, kf, vf, wk, wv, jnp.swapaxes(fm, 1, 2), jnp.swapaxes(sm, 1, 2))
    placed = [pltpu.with_memory_space_constraint(a, pltpu.HBM) for a in args]
    gat, wall, first, second = pl.pallas_call(
        functools.partial(kernel, n_fs, n_tp),
        out_shape=(
            pltpu.VMEM((n_fs, 2, rank, rows), BF16),
            pltpu.VMEM((n_fs, rows, nk + nv), BF16),
            pltpu.VMEM((2, r, rows), F32),
            pltpu.VMEM((2, r, rows), F32),
        ),
        in_specs=[pl.BlockSpec(memory_space=pltpu.HBM)] * 9,
        out_specs=(vmem,) * 4,
        scratch_shapes=[pltpu.VMEM(a.shape, a.dtype) for a in args]
        + [
            pltpu.VMEM((n_tp, 2 * r, tokens), BF16),
            pltpu.VMEM((peers, 2 * r, tokens), BF16),
            pltpu.VMEM((n_fs, 2 * r, rows), BF16),
            pltpu.VMEM((n_fs, 2 * r, rows), BF16),
            pltpu.VMEM((8, 128), F32),
            pltpu.VMEM((n_dev - 1, 8, 128), F32),
            dma((9,)),
            dma((peers,)),
            dma((peers,)),
            dma((n_fs,)),
            dma((n_fs,)),
            dma,
            dma,
            dma((n_fs,)),
            dma((n_fs,)),
            dma((n_fs, n_tp)),
            dma((n_fs, n_tp)),
            dma((2, n_far)),
            dma((n_far,)),
            dma((n_far,)),
            dma((n_far,)),
        ],
        compiler_params=pltpu.CompilerParams(
            collective_id=0, has_side_effects=True, vmem_limit_bytes=40 * 1024 * 1024
        ),
    )(*placed)
    first, second, new_k, new_v, k_copy, v_copy = pl.pallas_call(
        functools.partial(results, n_fs),
        out_shape=(
            jax.ShapeDtypeStruct(first.shape, F32),
            jax.ShapeDtypeStruct(second.shape, F32),
            jax.ShapeDtypeStruct(wk.shape, F32),
            jax.ShapeDtypeStruct(wv.shape, F32),
            jax.ShapeDtypeStruct((model, nk), BF16),
            jax.ShapeDtypeStruct((model, nv), BF16),
        ),
        in_specs=[vmem] * 8,
        out_specs=(vmem,) * 4 + (anywhere,) * 2,
        scratch_shapes=[
            pltpu.VMEM((n_fs, rows, nk), BF16),
            pltpu.VMEM((n_fs, rows, nv), BF16),
            dma((n_fs,)),
            dma((n_fs,)),
        ],
        compiler_params=pltpu.CompilerParams(vmem_limit_bytes=32 * 1024 * 1024),
    )(gat, wall, first, second, kf, vf, wk, wv)
    return (
        jnp.swapaxes(first, 1, 2),
        jnp.swapaxes(second, 1, 2),
        new_k,
        new_v,
        k_copy,
        v_copy,
    )


def solution(mesh):
    placed = (
        P("fs", None),
        P("fs", "tp"),
        P("fs", "tp"),
        P("tp", None),
        P("tp", None),
        P("fs", "tp"),
        P("fs", "tp"),
        P(None, "fs", "tp"),
        P(None, "fs", "tp"),
    )
    return jax.shard_map(
        functools.partial(local, mesh.shape["fs"], mesh.shape["tp"]),
        mesh=mesh,
        in_specs=placed,
        out_specs=(
            P(None, "fs", "tp"),
            P(None, "fs", "tp"),
            P("fs", "tp"),
            P("fs", "tp"),
            P(None, "tp"),
            P(None, "tp"),
        ),
        check_vma=False,
    )
```

```python
import functools

import jax
import jax.numpy as jnp
from jax import lax
from jax.experimental import pallas as pl
from jax.experimental.pallas import tpu as pltpu
from jax.sharding import PartitionSpec as P

step_rate = 0.05
clip_target = 0.1
beta_first = 0.8
beta_second = 0.95
small_eps = 1e-08
norm_eps = 1e-06

MESH = pl.DeviceIdType.MESH
BF16 = jnp.bfloat16
F32 = jnp.float32


def flip(a):
    return jnp.transpose(a.astype(F32))


def start(c):
    c.start()


def finish(c):
    c.wait_send()


def kernel(n_fs, n_tp, *refs):
    hbm = refs[:9]
    gat_ref, wall_ref, first_ref, second_ref = refs[9:13]
    held_in = refs[13:22]
    x_ref, dk_ref, dv_ref, kf_ref, vf_ref, wk_ref, wv_ref, fm_ref, sm_ref = held_in
    part_ref, partin_ref, tok_ref, tokin_ref, sq_ref, sqin_ref = refs[22:28]
    in_sem, part_ss, part_rs, tok_ss, tok_rs, sq_ss, sq_rs = refs[28:35]
    gf_ss, gf_rs, gt_ss, gt_rs, w_ss, w_rs, wx_ss, wx_rs = refs[35:]
    fs = lax.axis_index("fs")
    tp = lax.axis_index("tp")
    n_dev = n_fs * n_tp
    lin = fs * n_tp + tp
    rank = kf_ref.shape[1]
    r = rank // n_tp
    rows = wk_ref.shape[0]
    nk = wk_ref.shape[1]
    nv = wv_ref.shape[1]
    model = x_ref.shape[1]
    pair = 2 if n_fs % 2 == 0 else 1
    n_far = n_fs // pair
    far = fs // pair
    near = fs % pair

    loads = [
        pltpu.make_async_copy(hbm[i], held_in[i], in_sem.at[i]) for i in range(9)
    ]
    for i in (3, 4, 1, 2, 5, 6, 0, 7, 8):
        loads[i].start()

    barrier = pltpu.get_barrier_semaphore()

    @pl.loop(1, n_dev)
    def _(k):
        other = lax.rem(lin + k, n_dev)
        pl.semaphore_signal(
            barrier,
            inc=1,
            device_id={"fs": other // n_tp, "tp": lax.rem(other, n_tp)},
            device_id_type=MESH,
        )

    for i in (3, 4, 1, 2):
        loads[i].wait()
    kft = flip(kf_ref[...]).astype(BF16)
    vft = flip(vf_ref[...]).astype(BF16)
    last = (((1,), (1,)), ((), ()))
    red_k = lax.dot_general(kft, dk_ref[...], last, preferred_element_type=F32)
    red_v = lax.dot_general(vft, dv_ref[...], last, preferred_element_type=F32)
    for j in range(n_tp):
        part_ref[j, :r, :] = red_k[j * r : (j + 1) * r].astype(BF16)
        part_ref[j, r:, :] = red_v[j * r : (j + 1) * r].astype(BF16)
    for i in (5, 6):
        loads[i].wait()
    wall_ref[fs, :, :nk] = wk_ref[...].astype(BF16)
    wall_ref[fs, :, nk:] = wv_ref[...].astype(BF16)

    pl.semaphore_wait(barrier, n_dev - 1)

    def part_copy(k):
        to = lax.rem(tp + k, n_tp)
        return pltpu.make_async_remote_copy(
            src_ref=part_ref.at[to],
            dst_ref=partin_ref.at[k - 1],
            send_sem=part_ss.at[k - 1],
            recv_sem=part_rs.at[k - 1],
            device_id={"tp": to},
            device_id_type=MESH,
        )

    parts = [part_copy(k) for k in range(1, n_tp)]
    for c in parts:
        c.start()

    def wall_hop(block_far, way):
        block = wall_ref.at[block_far * pair + near]
        return pltpu.make_async_remote_copy(
            src_ref=block,
            dst_ref=block,
            send_sem=w_ss.at[(way + 1) // 2, block_far],
            recv_sem=w_rs.at[block_far],
            device_id={"fs": (far + way) * pair + near},
            device_id_type=MESH,
        )

    def wall_pair(block_far):
        block = wall_ref.at[block_far * pair + near]
        return pltpu.make_async_remote_copy(
            src_ref=block,
            dst_ref=block,
            send_sem=wx_ss.at[block_far],
            recv_sem=wx_rs.at[block_far],
            device_id={"fs": far * pair + 1 - near},
            device_id_type=MESH,
        )

    def wall_step(d, act):
        for way in (1, -1):
            block_far = far - d * way
            here = (block_far >= 0) & (block_far < n_far)
            more = here & (far + way >= 0) & (far + way < n_far)
            if d == 0:
                if pair == 2 and way == 1:
                    act(wall_pair(far))
            else:

                @pl.when(here)
                def _():
                    block = wall_ref.at[block_far * pair + near]
                    if act is start:
                        pltpu.make_async_copy(block, block, w_rs.at[block_far]).wait()

            @pl.when(more)
            def _():
                act(wall_hop(block_far, way))

            if d and pair == 2:

                @pl.when(here)
                def _():
                    act(wall_pair(block_far))

    wall_step(0, start)

    for c in parts:
        c.wait_recv()
    own = part_ref[tp].astype(F32)
    for k in range(1, n_tp):
        own = own + partin_ref[k - 1].astype(F32)
    own = own.astype(BF16)
    loads[0].wait()

    def tok_copy(c):
        return pltpu.make_async_remote_copy(
            src_ref=tok_ref.at[c],
            dst_ref=tokin_ref.at[fs],
            send_sem=tok_ss.at[c],
            recv_sem=tok_rs.at[fs],
            device_id={"fs": c},
            device_id_type=MESH,
        )

    width = max(rows, min(256, model))
    for base in range(0, model, width):
        prod = lax.dot_general(
            own,
            x_ref[:, base : base + width],
            (((1,), (0,)), ((), ())),
            preferred_element_type=F32,
        )
        for c in range(base // rows, (base + width) // rows):
            at = c * rows - base
            tok_ref[c] = prod[:, at : at + rows].astype(BF16)

            @pl.when(c != fs)
            def _():
                tok_copy(c).start()

    if n_far > 1:
        wall_step(1, start)
    for i in (7, 8):
        loads[i].wait()
    fmt = fm_ref[...].reshape(2 * r, rows)
    smt = sm_ref[...].reshape(2 * r, rows)

    total = tok_ref[fs].astype(F32)
    for k in range(1, n_fs):
        origin = lax.rem(fs + k, n_fs)
        pltpu.make_async_copy(
            tokin_ref.at[origin], tokin_ref.at[origin], tok_rs.at[origin]
        ).wait()
        total = total + tokin_ref[origin].astype(F32)

    sq_ref[...] = jnp.full(sq_ref.shape, jnp.sum(total * total), F32)

    def sq_copy(k):
        other = lax.rem(lin + k, n_dev)
        return pltpu.make_async_remote_copy(
            src_ref=sq_ref,
            dst_ref=sqin_ref.at[k - 1],
            send_sem=sq_ss,
            recv_sem=sq_rs,
            device_id={"fs": other // n_tp, "tp": lax.rem(other, n_tp)},
            device_id_type=MESH,
        )

    @pl.loop(1, n_dev)
    def _(k):
        sq_copy(k).start()

    if n_far > 2:
        wall_step(2, start)
    pltpu.make_async_copy(sqin_ref, sqin_ref, sq_rs).wait()
    total_sq = jnp.max(jnp.sum(sqin_ref[...], axis=0) + sq_ref[...])
    limit = clip_target * (2.0 * model * rank) ** 0.5
    clip_factor = jnp.minimum(
        1.0, limit / jnp.sqrt(jnp.full((1, 1), total_sq + norm_eps, F32))
    )
    scaled = clip_factor * total
    first_new = beta_first * fmt + (1.0 - beta_first) * scaled
    second_new = beta_second * smt + (1.0 - beta_second) * scaled * scaled
    direction = first_new / (jnp.sqrt(second_new) + small_eps)

    mine = pl.ds(pl.multiple_of(tp * r, r), r)
    gat_ref[fs, 0, mine, :] = direction[:r].astype(BF16)
    gat_ref[fs, 1, mine, :] = direction[r:].astype(BF16)

    def gat_copy(k):
        block = gat_ref.at[fs, :, mine, :]
        return pltpu.make_async_remote_copy(
            src_ref=block,
            dst_ref=block,
            send_sem=gf_ss.at[k - 1],
            recv_sem=gf_rs.at[k - 1],
            device_id={"fs": lax.rem(fs + k, n_fs)},
            device_id_type=MESH,
        )

    def gat_in(k):
        origin = lax.rem(fs + n_fs - k, n_fs)
        block = gat_ref.at[origin, :, mine, :]
        return pltpu.make_async_copy(block, block, gf_rs.at[k - 1])

    bits = []
    b = n_tp // 2
    while b:
        bits.append(b)
        b //= 2

    def flipped(v, bit):
        return v + bit - 2 * bit * (v // bit % 2)

    held = [[]]
    for bit in bits:
        held.append(held[-1] + [bit])

    def sources(step):
        out = [0]
        for bit in bits[:step]:
            out = out + [o + bit for o in out]
        return out

    def tp_of(mask):
        v = tp
        for bit in bits:
            if mask & bit:
                v = flipped(v, bit)
        return v

    def share_copy(k, step, mask):
        origin = lax.rem(fs + n_fs - k, n_fs)
        at = pl.ds(pl.multiple_of(tp_of(mask) * r, r), r)
        block = gat_ref.at[origin, :, at, :]
        slot = mask | bits[step]
        return pltpu.make_async_remote_copy(
            src_ref=block,
            dst_ref=block,
            send_sem=gt_ss.at[k, slot - 1],
            recv_sem=gt_rs.at[k, slot - 1],
            device_id={"tp": flipped(tp, bits[step])},
            device_id_type=MESH,
        )

    def share_in(k, slot):
        origin = lax.rem(fs + n_fs - k, n_fs)
        at = pl.ds(pl.multiple_of(tp_of(slot) * r, r), r)
        block = gat_ref.at[origin, :, at, :]
        return pltpu.make_async_copy(block, block, gt_rs.at[k, slot - 1])

    shares = []

    def share(k, step, mask):
        c = share_copy(k, step, mask)
        c.start()
        shares.append(c)

    gats = [gat_copy(k) for k in range(1, n_fs)]
    for step in range(len(bits)):
        share(0, step, 0)
    for c in gats:
        c.start()

    first_ref[...] = first_new.reshape(2, r, rows)
    second_ref[...] = second_new.reshape(2, r, rows)

    for d in range(3, n_far):
        wall_step(d, start)

    order = list(range(n_fs))
    for k in order:
        if k:
            gat_in(k).wait()
            for step in range(len(bits)):
                share(k, step, 0)
    for step in range(1, len(bits)):
        for k in order:
            for mask in sources(step - 1):
                got = mask | bits[step - 1]
                share_in(k, got).wait()
                for later in range(step, len(bits)):
                    share(k, later, got)
    for k in order:
        if bits:
            for mask in sources(len(bits) - 1):
                share_in(k, mask | bits[-1]).wait()
    if pair == 2:
        for m in range(n_far):
            block = wall_ref.at[m * pair + 1 - near]
            pltpu.make_async_copy(block, block, wx_rs.at[m]).wait()

    for c in parts + gats + shares:
        c.wait_send()
    for d in range(n_far):
        wall_step(d, finish)
    for c in range(n_fs):

        @pl.when(c != fs)
        def _():
            tok_copy(c).wait_send()

    pltpu.make_async_copy(sqin_ref, sqin_ref, sq_ss).wait()


def results(
    n_fs,
    gat_ref,
    wall_ref,
    first_in,
    second_in,
    kf_ref,
    vf_ref,
    wk_ref,
    wv_ref,
    first_ref,
    second_ref,
    newk_ref,
    newv_ref,
    kout_ref,
    vout_ref,
    kcopy_ref,
    vcopy_ref,
    k_sem,
    v_sem,
):
    fs = lax.axis_index("fs")
    rows, nk = wk_ref.shape
    back = (((0,), (0,)), ((), ()))
    kft = flip(kf_ref[...]).astype(BF16)
    vft = flip(vf_ref[...]).astype(BF16)
    first_ref[...] = first_in[...]
    second_ref[...] = second_in[...]

    def update(block):
        up_k = lax.dot_general(gat_ref[block, 0], kft, back, preferred_element_type=F32)
        up_v = lax.dot_general(gat_ref[block, 1], vft, back, preferred_element_type=F32)
        return step_rate * up_k, step_rate * up_v

    outs = []
    for k in range(n_fs):
        origin = lax.rem(fs + k, n_fs)
        up_k, up_v = update(origin)
        at = pl.ds(pl.multiple_of(origin * rows, rows), rows)
        if k == 0:
            new_k = wk_ref[...] - up_k
            new_v = wv_ref[...] - up_v
            newk_ref[...] = new_k
            newv_ref[...] = new_v
        else:
            new_k = wall_ref[origin, :, :nk].astype(F32) - up_k
            new_v = wall_ref[origin, :, nk:].astype(F32) - up_v
        kcopy_ref[k] = new_k.astype(BF16)
        vcopy_ref[k] = new_v.astype(BF16)
        for c in (
            pltpu.make_async_copy(kcopy_ref.at[k], kout_ref.at[at, :], k_sem.at[k]),
            pltpu.make_async_copy(vcopy_ref.at[k], vout_ref.at[at, :], v_sem.at[k]),
        ):
            c.start()
            outs.append(c)
    for c in outs:
        c.wait()


def local(n_fs, n_tp, x, dk, dv, kf, vf, wk, wv, fm, sm):
    tokens, model = x.shape
    rows, nk = wk.shape
    nv = wv.shape[1]
    rank = kf.shape[1]
    r = rank // n_tp
    n_dev = n_fs * n_tp
    dma = pltpu.SemaphoreType.DMA
    vmem = pl.BlockSpec(memory_space=pltpu.VMEM)
    anywhere = pl.BlockSpec(memory_space=pl.ANY)
    pair = 2 if n_fs % 2 == 0 else 1
    n_far = n_fs // pair
    peers = max(n_tp - 1, 1)
    args = (x, dk, dv, kf, vf, wk, wv, jnp.swapaxes(fm, 1, 2), jnp.swapaxes(sm, 1, 2))
    placed = [pltpu.with_memory_space_constraint(a, pltpu.HBM) for a in args]
    gat, wall, first, second = pl.pallas_call(
        functools.partial(kernel, n_fs, n_tp),
        out_shape=(
            pltpu.VMEM((n_fs, 2, rank, rows), BF16),
            pltpu.VMEM((n_fs, rows, nk + nv), BF16),
            pltpu.VMEM((2, r, rows), F32),
            pltpu.VMEM((2, r, rows), F32),
        ),
        in_specs=[pl.BlockSpec(memory_space=pltpu.HBM)] * 9,
        out_specs=(vmem,) * 4,
        scratch_shapes=[pltpu.VMEM(a.shape, a.dtype) for a in args]
        + [
            pltpu.VMEM((n_tp, 2 * r, tokens), BF16),
            pltpu.VMEM((peers, 2 * r, tokens), BF16),
            pltpu.VMEM((n_fs, 2 * r, rows), BF16),
            pltpu.VMEM((n_fs, 2 * r, rows), BF16),
            pltpu.VMEM((1, 128), F32),
            pltpu.VMEM((n_dev - 1, 1, 128), F32),
            dma((9,)),
            dma((peers,)),
            dma((peers,)),
            dma((n_fs,)),
            dma((n_fs,)),
            dma,
            dma,
            dma((n_fs,)),
            dma((n_fs,)),
            dma((n_fs, n_tp)),
            dma((n_fs, n_tp)),
            dma((2, n_far)),
            dma((n_far,)),
            dma((n_far,)),
            dma((n_far,)),
        ],
        compiler_params=pltpu.CompilerParams(
            collective_id=0, has_side_effects=True, vmem_limit_bytes=40 * 1024 * 1024
        ),
    )(*placed)
    first, second, new_k, new_v, k_copy, v_copy = pl.pallas_call(
        functools.partial(results, n_fs),
        out_shape=(
            jax.ShapeDtypeStruct(first.shape, F32),
            jax.ShapeDtypeStruct(second.shape, F32),
            jax.ShapeDtypeStruct(wk.shape, F32),
            jax.ShapeDtypeStruct(wv.shape, F32),
            jax.ShapeDtypeStruct((model, nk), BF16),
            jax.ShapeDtypeStruct((model, nv), BF16),
        ),
        in_specs=[vmem] * 8,
        out_specs=(vmem,) * 4 + (anywhere,) * 2,
        scratch_shapes=[
            pltpu.VMEM((n_fs, rows, nk), BF16),
            pltpu.VMEM((n_fs, rows, nv), BF16),
            dma((n_fs,)),
            dma((n_fs,)),
        ],
        compiler_params=pltpu.CompilerParams(vmem_limit_bytes=32 * 1024 * 1024),
    )(gat, wall, first, second, kf, vf, wk, wv)
    return (
        jnp.swapaxes(first, 1, 2),
        jnp.swapaxes(second, 1, 2),
        new_k,
        new_v,
        k_copy,
        v_copy,
    )


def solution(mesh):
    placed = (
        P("fs", None),
        P("fs", "tp"),
        P("fs", "tp"),
        P("tp", None),
        P("tp", None),
        P("fs", "tp"),
        P("fs", "tp"),
        P(None, "fs", "tp"),
        P(None, "fs", "tp"),
    )
    return jax.shard_map(
        functools.partial(local, mesh.shape["fs"], mesh.shape["tp"]),
        mesh=mesh,
        in_specs=placed,
        out_specs=(
            P(None, "fs", "tp"),
            P(None, "fs", "tp"),
            P("fs", "tp"),
            P("fs", "tp"),
            P(None, "tp"),
            P(None, "tp"),
        ),
        check_vma=False,
    )
```
